32 devices in a mesh: sp: 4 (over y, x), tp: 8 (over z, core).
Axes of the slice: x: 2, y: 2, z: 4, core: 2. Of those that a mesh axis runs over, the one named last changes fastest.
Arguments:
- upstream: bfloat16 [1024, 4096], P('sp', 'tp'), may hold values from -6 to 6
- stream: bfloat16 [1024, 4096], P('sp', 'tp'), may hold values from -400 to 400
- norm_gain: float32 [4096], P('tp'), may hold values from 0.1 to 1.9
- routes: int32 [1024, 2], P('sp'), may hold values from 0 to 3, all different within a row; in each aligned block of 256 rows (0 to 255, 256 to 511, ...) at most 192 rows name the same one
- route_weights: float32 [1024, 2], P('sp'), may hold values from 0.1 to 1
- w_gate: bfloat16 [4, 4096, 2048], P('sp', None, 'tp'), may hold values from -0.09375 to 0.09375
- w_up: bfloat16 [4, 4096, 2048], P('sp', None, 'tp'), may hold values from -0.09375 to 0.09375
- w_down: bfloat16 [4, 2048, 4096], P('sp', 'tp'), may hold values from -0.125 to 0.125
- value_in: bfloat16 [1024, 2048], P('sp', 'tp'), may hold values from -6 to 6
- gate_in: bfloat16 [1024, 2048], P('sp', 'tp'), may hold values from -6 to 6
- conv_pre: bfloat16 [1024, 2048], P('sp', 'tp'), may hold values from -200 to 200
- ln_gain: float32 [2048], P('tp'), may hold values from 0.1 to 1.9
- conv_taps: float32 [31, 2048], P(None, 'tp'), may hold values from -1 to 1
- w_out: bfloat16 [2048, 4096], P('tp'), may hold values from -0.125 to 0.125
Outputs:
- grad_gate: float32 [4, 4096, 2048], P('sp', None, 'tp')
- grad_up: float32 [4, 4096, 2048], P('sp', None, 'tp')
- grad_down: float32 [4, 2048, 4096], P('sp', 'tp')
- grad_out: float32 [2048, 4096], P('tp', 'sp')
- value_grad: bfloat16 [1024, 2048], P('sp', 'tp')
- gate_grad: bfloat16 [1024, 2048], P('sp', 'tp')
The draws below stay inside these ranges and needn't reach their ends.
Inputs may be any that keep to these rules, and one draw needn't show every extreme that they name: `routes`: each token names two different experts. Among the tokens of one index of sp no expert is named more than 192 times, and in every draw some expert exactly 192 times.
All inputs are finite; a program needn't handle non-finite values.
Results may differ from the reference program's by a relative error of at most 0.0071.
Values may be sent and summed in bfloat16 or wider, within the bound.
A program may use at most 128 MiB of HBM per device.

```python
import math
import jax
import jax.numpy as jnp
import numpy as np
from jax import lax

D = 4096
C = 2048
FF = 2048
TAPS = 31
TOK_DEV = 256
TOKENS = 1024
EXPERTS = 4
CAP = 192
N_SP = 4


def draw_stream(key, part):
    subkeys = jax.random.split(jax.random.fold_in(key, 11), 3)
    random_part = jnp.clip(jax.random.normal(subkeys[0], (TOKENS, D), jnp.float32), -6.0, 6.0)
    row_scale = jnp.exp(jax.random.uniform(subkeys[1], (TOKENS, 1), jnp.float32, 0.0, math.log(10.0)))
    rising = jnp.exp(math.log(10.0) * (jnp.arange(D, dtype=jnp.float32) + 0.5) / D)
    jitter = jnp.exp(jax.random.uniform(subkeys[2], (D,), jnp.float32, -0.3, 0.3))
    column_scale = rising * jitter
    return (random_part * row_scale * column_scale[None, :] / 3.0).astype(jnp.bfloat16)


def draw_conv_pre(key, part):
    subkeys = jax.random.split(jax.random.fold_in(key, 23), 4)
    random_part = jnp.clip(jax.random.normal(subkeys[0], (TOKENS, C), jnp.float32), -6.0, 6.0)
    row_scale = jnp.exp(jax.random.uniform(subkeys[1], (TOKENS, 1), jnp.float32, 0.0, math.log(4.0)))
    rising = jnp.exp(math.log(10.0) * (jnp.arange(C, dtype=jnp.float32) + 0.5) / C)
    jitter = jnp.exp(jax.random.uniform(subkeys[2], (C,), jnp.float32, -0.3, 0.3))
    column_scale = rising * jitter
    row_offset = 1.5 * jnp.clip(jax.random.normal(subkeys[3], (TOKENS, 1), jnp.float32), -3.0, 3.0)
    return ((random_part * column_scale[None, :] / 3.0 + row_offset) * row_scale).astype(jnp.bfloat16)


def with_spikes(entries, rng, source, target, blocks, factor):
    def block_of(position):
        return (jnp.arange(entries.shape[position]) // (entries.shape[position] // blocks)).reshape((-1,) + (1,) * (entries.ndim - 1 - position))

    first = jax.random.permutation(rng, blocks)[block_of(target)]
    other_side = (block_of(target) + blocks // 2) % blocks
    return jnp.where((block_of(source) == first) | (block_of(source) == other_side), factor * entries, entries)


def block_levels(own_key, dims, pieces, low, top_value):
    def one(position, blocks):
        draws = jax.random.uniform(jax.random.fold_in(jax.random.fold_in(own_key, 6), position), (blocks,), jnp.float32, low / len(pieces), top_value / len(pieces))
        return jnp.repeat(jnp.exp(draws), dims[position] // blocks).reshape((-1,) + (1,) * (len(dims) - position - 1))

    gain = one(*pieces[0])
    for cut in pieces[1:]:
        gain = gain * one(*cut)
    return gain


def assign_block(key, own, number, rows, count, top, reach, slope):
    sequence = jax.random.permutation(key, count)
    packed, common = shares(count, rows * top, reach, slope, True), shares(count, rows * top, reach, slope, False)
    places = jnp.arange(count)

    def named(sizes, turn):
        used = int((sizes > 0).sum())
        fixed = max(1, used // 4)
        shifted = fixed + (places - fixed + turn * (used - fixed)) % max(1, count - fixed)
        return jnp.zeros((count,), jnp.int32).at[sequence[jnp.where(places < fixed, places, shifted)]].set(jnp.asarray(sizes, jnp.int32))

    sizes = jnp.where(number % 4 == 0, named(packed, number // 4), named(common, number - number // 4 - 1))
    mixed = jax.random.permutation(jax.random.fold_in(own, 3), count)
    source_of, receiver = mixed[0:count // 2 * 2:2], mixed[1:count // 2 * 2:2]
    room = jnp.minimum(sizes[source_of] - 1, reach - sizes[receiver]) // 2
    room = jnp.where((source_of == sequence[0]) | (receiver == sequence[0]) | (sizes[receiver] == 0), 0, jnp.maximum(room, 0))
    shifted = jax.random.randint(jax.random.fold_in(own, 4), (count // 2,), 0, 1 << 20) % (room + 1)
    sizes = sizes.at[source_of].add(-shifted).at[receiver].add(shifted)
    labels = jnp.searchsorted(jnp.cumsum(sizes), jnp.arange(rows * top), side="right").astype(jnp.int32)
    listing = labels.reshape(top, rows).T
    listing = listing[jax.random.permutation(jax.random.fold_in(own, 1), rows)]
    turn = jax.random.randint(jax.random.fold_in(own, 2), (rows, 1), 0, top)
    return jnp.take_along_axis(listing, (jnp.arange(top)[None, :] + turn) % top, axis=1)


def shares(number_of, total, reach, lean, full):
    loads = [(1 << 20) // math.isqrt(grade ** lean) + 1 for grade in range(1, number_of + 1)]
    largest = reach if full else min(reach, max(-(-total // number_of), total * loads[0] // sum(loads)))
    least = 1 if total - largest >= number_of - 1 else 0
    holding, rest = [largest] + [least] * (number_of - 1), total - largest - least * (number_of - 1)
    while rest > 0:
        candidates = [i for i in range(1, number_of) if holding[i] < largest] or [i for i in range(1, number_of) if holding[i] < reach]
        whole, left = sum([loads[i] for i in candidates]), rest
        for i in candidates:
            addition = min(reach - holding[i], max(1, left * loads[i] // whole), rest)
            holding[i] = holding[i] + addition
            rest = rest - addition
    return np.array(holding)


def scatter_about(own_key, extent, width, limit, pieces=(), kind=jnp.bfloat16):
    values = jax.random.normal(own_key, extent, jnp.float32) * width
    if len(pieces) > 0:
        values = block_levels(own_key, extent, pieces, -0.22, 0.18) * values
    return jnp.clip(values, min=-limit, max=limit).astype(kind)


def bell_draw_with(own_key, extent, scale, most, cuts, heavy, held_as=jnp.bfloat16):
    drawn = scale * jax.random.normal(own_key, extent, jnp.float32)
    if cuts:
        drawn = drawn * block_levels(own_key, extent, cuts, -0.22, 0.18)
    return jnp.clip(with_spikes(drawn, jax.random.fold_in(own_key, 3), *heavy), -most, most).astype(held_as)


def setup_inputs(seed: int = 0) -> dict:
    splits = jax.random.split(jax.random.key(seed), 15)
    upstream = bell_draw_with(splits[0], (TOKENS, D), 1.0, 6.0, ((0, 4), (1, 8)), (0, 1, 8, 2.0))
    stream = draw_stream(jax.random.fold_in(splits[14], 71), 0)
    norm_gain = jnp.clip(1.0 + 0.18 * jax.random.normal(splits[2], (D,), jnp.float32), 0.1, 1.9)
    routes_keys = jax.random.split(jax.random.fold_in(splits[3], 1), TOKENS // TOK_DEV)
    routes_turns = jax.random.permutation(jax.random.fold_in(splits[3], 3), TOKENS // TOK_DEV)
    routes = jax.vmap(lambda own, number: assign_block(jax.random.fold_in(splits[3], 2), own, number, TOK_DEV, EXPERTS, 2, CAP, 1))(routes_keys, routes_turns).reshape((TOKENS, 2))
    route_weights = jnp.clip(jnp.exp(math.log(1.0) - 2.3025851 * jax.random.uniform(splits[4], (TOKENS, 2), jnp.float32) ** block_levels(splits[4], (TOKENS, 2), ((0, 4),), -0.2, 0.2)), 0.1, 1.0)
    w_gate = scatter_about(splits[5], (EXPERTS, D, FF), D ** -0.5, 0.09375, ((0, 4), (2, 8)))
    w_up = scatter_about(splits[6], (EXPERTS, D, FF), D ** -0.5, 0.09375, ((0, 4), (2, 8)))
    w_down = scatter_about(splits[7], (EXPERTS, FF, D), FF ** -0.5, 0.125, ((0, 4), (1, 8)))
    value_in = scatter_about(splits[8], (TOKENS, C), 1.0, 6.0, ((0, 4), (1, 8)))
    gate_in = scatter_about(splits[9], (TOKENS, C), 1.5, 6.0, ((0, 4), (1, 8)))
    conv_pre = draw_conv_pre(jax.random.fold_in(splits[14], 71), 0)
    ln_gain = jnp.clip(1.0 + 0.18 * jax.random.normal(splits[11], (C,), jnp.float32), 0.1, 1.9)
    conv_taps = scatter_about(splits[12], (TAPS, C), TAPS ** -0.5, 1.0, ((1, 8),), jnp.float32)
    w_out = scatter_about(splits[13], (C, D), C ** -0.5, 0.125, ((0, 8),))
    return dict(upstream=upstream, stream=stream, norm_gain=norm_gain, routes=routes, route_weights=route_weights, w_gate=w_gate, w_up=w_up, w_down=w_down, value_in=value_in, gate_in=gate_in, conv_pre=conv_pre, ln_gain=ln_gain, conv_taps=conv_taps, w_out=w_out)


EPSILON = 1e-06

def silu_slope(values):
    logistic = jax.nn.sigmoid(values)
    return logistic * (1.0 + values * (1.0 - logistic))

def reference(upstream, stream, norm_gain, routes, route_weights, w_gate, w_up, w_down, value_in, gate_in, conv_pre, ln_gain, conv_taps, w_out):
    tokens, model_width = stream.shape
    experts = w_gate.shape[0]
    channels = conv_pre.shape[1]
    tap_count = conv_taps.shape[0]
    capacity = 3 * TOK_DEV // N_SP
    expert_rows = N_SP * capacity
    residual = stream.astype(jnp.float32)
    inverse = lax.rsqrt(lax.optimization_barrier(jnp.mean(residual * residual, axis=1, keepdims=True)) + EPSILON)
    normed = (norm_gain[None, :] * residual * inverse).astype(jnp.bfloat16)
    flat_experts = routes.reshape(-1)
    one_hot = (flat_experts[:, None] == jnp.arange(experts, dtype=jnp.int32)[None, :]).astype(jnp.int32)
    blocked = one_hot.reshape(N_SP, 2 * TOK_DEV, experts)
    earlier = (jnp.cumsum(blocked, axis=1) - blocked) * blocked
    slot_rank = lax.optimization_barrier(jnp.sum(earlier, axis=2)).reshape(-1)
    source = jnp.arange(2 * tokens, dtype=jnp.int32) // (2 * TOK_DEV)
    slot_index = flat_experts * expert_rows + source * capacity + slot_rank
    token_of = jnp.full((experts * expert_rows,), tokens, jnp.int32).at[slot_index].set(jnp.arange(2 * tokens, dtype=jnp.int32) // 2)
    weight_of = jnp.zeros((experts * expert_rows,), jnp.float32).at[slot_index].set(route_weights.reshape(-1))
    normed_pad = jnp.concatenate([normed, jnp.zeros((1, model_width), jnp.bfloat16)], axis=0)
    upstream_pad = jnp.concatenate([upstream, jnp.zeros((1, model_width), jnp.bfloat16)], axis=0)

    def one_expert(operands):
        indices, weights, gate_mat, upper_mat, down_mat = operands
        inputs = normed_pad[indices]
        cotangent = (weights[:, None] * upstream_pad[indices].astype(jnp.float32)).astype(jnp.bfloat16)
        gate_pre = jnp.dot(inputs, gate_mat, preferred_element_type=jnp.float32)
        upper_pre = jnp.dot(inputs, upper_mat, preferred_element_type=jnp.float32)
        active = (jax.nn.silu(gate_pre) * upper_pre).astype(jnp.bfloat16)
        active_back = jnp.dot(cotangent, down_mat.T, preferred_element_type=jnp.float32)
        gate_back = (active_back * upper_pre * silu_slope(gate_pre)).astype(jnp.bfloat16)
        upper_back = (active_back * jax.nn.silu(gate_pre)).astype(jnp.bfloat16)
        grad_gate = jnp.dot(inputs.T, gate_back, preferred_element_type=jnp.float32)
        grad_up = jnp.dot(inputs.T, upper_back, preferred_element_type=jnp.float32)
        grad_down = jnp.dot(active.T, cotangent, preferred_element_type=jnp.float32)
        input_back = (jnp.dot(gate_back, gate_mat.T, preferred_element_type=jnp.float32) + jnp.dot(upper_back, upper_mat.T, preferred_element_type=jnp.float32)).astype(jnp.bfloat16)
        return (grad_gate, grad_up, grad_down, input_back)
    grad_gate, grad_up, grad_down, input_back = lax.map(one_expert, (token_of.reshape(experts, expert_rows), weight_of.reshape(experts, expert_rows), w_gate, w_up, w_down))
    token_back = jnp.zeros((tokens + 1, model_width), jnp.float32).at[token_of].add(input_back.reshape(-1, model_width).astype(jnp.float32))[:tokens]
    gained = norm_gain[None, :] * token_back
    inner_sum = lax.optimization_barrier(jnp.sum(gained * residual, axis=1, keepdims=True))
    norm_back = inverse * gained - residual * inverse ** 3 * inner_sum / model_width
    stream_grad = (upstream.astype(jnp.float32) + norm_back).astype(jnp.bfloat16)
    conv_vals = conv_pre.astype(jnp.float32)
    mean_val = lax.optimization_barrier(jnp.mean(conv_vals, axis=1, keepdims=True))
    variance = lax.optimization_barrier(jnp.mean(conv_vals * conv_vals, axis=1, keepdims=True)) - mean_val * mean_val
    inv_std = lax.rsqrt(variance + EPSILON)
    centred = (conv_vals - mean_val) * inv_std
    scaled = centred * ln_gain[None, :]
    mixed_out = jax.nn.silu(scaled).astype(jnp.bfloat16)
    grad_out = jnp.dot(mixed_out.T, stream_grad, preferred_element_type=jnp.float32)
    mixed_back = jnp.dot(stream_grad, w_out.T, preferred_element_type=jnp.float32)
    norm_in = mixed_back * silu_slope(scaled) * ln_gain[None, :]
    conv_back = inv_std * (norm_in - lax.optimization_barrier(jnp.mean(norm_in, axis=1, keepdims=True)) - centred * lax.optimization_barrier(jnp.mean(norm_in * centred, axis=1, keepdims=True)))
    padded = jnp.concatenate([conv_back, jnp.zeros((tap_count - 1, channels), jnp.float32)], axis=0)
    glu_back = jnp.zeros((tokens, channels), jnp.float32)
    for tap_index in range(tap_count):
        offset = tap_count - 1 - tap_index
        glu_back = glu_back + conv_taps[tap_index][None, :] * padded[offset:offset + tokens]
    gate_sigma = jax.nn.sigmoid(gate_in.astype(jnp.float32))
    value_grad = (glu_back * gate_sigma).astype(jnp.bfloat16)
    gate_grad = (glu_back * value_in.astype(jnp.float32) * gate_sigma * (1.0 - gate_sigma)).astype(jnp.bfloat16)
    return (grad_gate, grad_up, grad_down, grad_out, value_grad, gate_grad)
```

```python
import functools

import jax
import jax.numpy as jnp
from jax import lax
from jax.experimental import pallas as pl
from jax.experimental.pallas import tpu as pltpu
from jax.sharding import PartitionSpec as P

EPSILON = 1e-06


def shifted(block, axis, distance):
    devices = range(lax.axis_size(axis))
    route = [(i - distance, i) for i in devices if i - distance in devices]
    return lax.ppermute(block, axis, route)


def group_sum_kernel(axis, group, own_ref, out_ref, landed, send_sems, recv_sems):
    me = lax.axis_index(axis)
    barrier = pltpu.get_barrier_semaphore()
    for step in range(1, group):
        pl.semaphore_signal(
            barrier,
            inc=1,
            device_id={axis: lax.rem(me + step, group)},
            device_id_type=pl.DeviceIdType.MESH,
        )
    pl.semaphore_wait(barrier, group - 1)
    copies = []
    for step in range(1, group):
        copy = pltpu.make_async_remote_copy(
            src_ref=own_ref,
            dst_ref=landed.at[step - 1],
            send_sem=send_sems.at[step - 1],
            recv_sem=recv_sems.at[step - 1],
            device_id={axis: lax.rem(me + step, group)},
            device_id_type=pl.DeviceIdType.MESH,
        )
        copy.start()
        copies.append(copy)
    for copy in copies:
        copy.wait()
    total = own_ref[...]
    for step in range(1, group):
        total = total + landed[step - 1]
    out_ref[...] = total


def group_sum(vectors, axis, collective_id):
    block = jnp.stack(vectors, axis=0)
    group = lax.axis_size(axis)
    summed = pl.pallas_call(
        functools.partial(group_sum_kernel, axis, group),
        out_shape=jax.ShapeDtypeStruct(block.shape, block.dtype),
        in_specs=[pl.BlockSpec(memory_space=pltpu.VMEM)],
        out_specs=pl.BlockSpec(memory_space=pltpu.VMEM),
        scratch_shapes=[
            pltpu.VMEM((group - 1,) + block.shape, block.dtype),
            pltpu.SemaphoreType.DMA((group - 1,)),
            pltpu.SemaphoreType.DMA((group - 1,)),
        ],
        compiler_params=pltpu.CompilerParams(
            collective_id=collective_id, has_side_effects=True
        ),
        cost_estimate=pl.CostEstimate(
            flops=group * block.size, bytes_accessed=400 * block.size * 4, transcendentals=0
        ),
        name="group_sum",
    )(block)
    return tuple(summed[row] for row in range(len(vectors)))


def silu_slope(values):
    logistic = jax.nn.sigmoid(values)
    return logistic * (1.0 + values * (1.0 - logistic))


def per_device(
    upstream,
    stream,
    norm_gain,
    routes,
    route_weights,
    w_gate,
    w_up,
    w_down,
    value_in,
    gate_in,
    conv_pre,
    ln_gain,
    conv_taps,
    w_out,
):
    tok_rows, width_part = stream.shape
    token_groups = lax.axis_size("sp")
    width_groups = lax.axis_size("tp")
    model_width = width_part * width_groups
    channels = conv_pre.shape[1] * width_groups
    tap_count = conv_taps.shape[0]
    capacity = 3 * tok_rows // token_groups
    experts = w_gate.shape[0] * token_groups
    slot_count = experts * capacity
    expert_rows = token_groups * capacity
    flat_experts = routes.reshape(-1)
    one_hot = (flat_experts[:, None] == jnp.arange(experts, dtype=jnp.int32)[None, :]).astype(
        jnp.int32
    )
    slot_rank = jnp.sum((jnp.cumsum(one_hot, axis=0) - one_hot) * one_hot, axis=1)
    slot_index = (flat_experts * capacity + slot_rank).reshape(tok_rows, 2)
    slot_ids = jnp.arange(slot_count, dtype=jnp.int32)[:, None]
    first_hit = slot_ids == slot_index[None, :, 0]
    second_hit = slot_ids == slot_index[None, :, 1]
    any_hit = jnp.logical_or(first_hit, second_hit)
    picker = any_hit.astype(jnp.bfloat16)
    slot_weight = jnp.sum(
        jnp.where(first_hit, route_weights[None, :, 0], 0.0)
        + jnp.where(second_hit, route_weights[None, :, 1], 0.0),
        axis=1,
    )
    token_iota = jnp.arange(tok_rows, dtype=jnp.int32)[None, :]
    slot_token = jnp.where(
        jnp.any(any_hit, axis=1), jnp.sum(jnp.where(any_hit, token_iota, 0), axis=1), tok_rows
    )
    columns = stream.shape[1]
    spare = jnp.zeros((1, columns), jnp.bfloat16)
    upstream_pad = jnp.concatenate([upstream, spare], axis=0)
    cotangent = (upstream_pad[slot_token].astype(jnp.float32) * slot_weight[:, None]).astype(
        jnp.bfloat16
    )
    sent_cotangent = cotangent.reshape(experts, capacity, columns)
    part_cotangent = lax.all_to_all(
        sent_cotangent, "sp", split_axis=0, concat_axis=0, tiled=True
    ).reshape(expert_rows, width_part)
    part_cotangent, stream_late, conv_late = lax.optimization_barrier(
        (part_cotangent, stream, conv_pre)
    )
    cotangent = lax.all_gather(part_cotangent, "tp", axis=1, tiled=True)
    residual = stream_late.astype(jnp.float32)
    conv_vals = conv_late.astype(jnp.float32)
    row_squares, conv_total, conv_squares = group_sum(
        (
            jnp.sum(residual * residual, axis=1),
            jnp.sum(conv_vals, axis=1),
            jnp.sum(conv_vals * conv_vals, axis=1),
        ),
        "tp",
        0,
    )
    inverse = lax.rsqrt(row_squares / model_width + EPSILON)[:, None]
    normed = (norm_gain[None, :] * residual * inverse).astype(jnp.bfloat16)
    normed_pad = jnp.concatenate([normed, spare], axis=0)
    inputs = normed_pad[slot_token]
    sent_inputs = inputs.reshape(experts, capacity, columns)
    part_inputs = lax.all_to_all(sent_inputs, "sp", split_axis=0, concat_axis=0, tiled=True)
    inputs = lax.all_gather(
        part_inputs.reshape(expert_rows, width_part), "tp", axis=1, tiled=True
    )
    gate_mat = w_gate[0]
    upper_mat = w_up[0]
    down_mat = w_down[0]
    gate_pre = jnp.dot(inputs, gate_mat, preferred_element_type=jnp.float32)
    upper_pre = jnp.dot(inputs, upper_mat, preferred_element_type=jnp.float32)
    active = (jax.nn.silu(gate_pre) * upper_pre).astype(jnp.bfloat16)
    active_back = lax.dot_general(
        cotangent, down_mat, (((1,), (1,)), ((), ())), preferred_element_type=jnp.float32
    )
    gate_back = (active_back * upper_pre * silu_slope(gate_pre)).astype(jnp.bfloat16)
    upper_back = (active_back * jax.nn.silu(gate_pre)).astype(jnp.bfloat16)
    grad_gate = lax.dot_general(
        inputs, gate_back, (((0,), (0,)), ((), ())), preferred_element_type=jnp.float32
    )
    grad_up = lax.dot_general(
        inputs, upper_back, (((0,), (0,)), ((), ())), preferred_element_type=jnp.float32
    )
    grad_down = lax.dot_general(
        active, cotangent, (((0,), (0,)), ((), ())), preferred_element_type=jnp.float32
    )
    input_part = lax.dot_general(
        gate_back, gate_mat, (((1,), (1,)), ((), ())), preferred_element_type=jnp.float32
    ) + lax.dot_general(
        upper_back, upper_mat, (((1,), (1,)), ((), ())), preferred_element_type=jnp.float32
    )
    input_back = lax.psum_scatter(
        input_part.astype(jnp.bfloat16), "tp", scatter_dimension=1, tiled=True
    )
    input_back, grad_gate, grad_up, grad_down = lax.optimization_barrier(
        (input_back, grad_gate, grad_up, grad_down)
    )
    returned = lax.all_to_all(
        input_back.reshape(token_groups, capacity, width_part),
        "sp",
        split_axis=0,
        concat_axis=0,
        tiled=True,
    )
    returned = returned.reshape(slot_count, width_part)
    token_back = lax.dot_general(
        picker, returned, (((0,), (0,)), ((), ())), preferred_element_type=jnp.float32
    )
    gained = norm_gain[None, :] * token_back
    (inner_sum,) = group_sum((jnp.sum(gained * residual, axis=1),), "tp", 1)
    norm_back = inverse * gained - residual * inverse**3 * (inner_sum / model_width)[:, None]
    stream_grad = (upstream.astype(jnp.float32) + norm_back).astype(jnp.bfloat16)
    full_grad = lax.all_gather(stream_grad, "tp", axis=1, tiled=True)
    mean_val = (conv_total / channels)[:, None]
    variance = (conv_squares / channels)[:, None] - mean_val * mean_val
    inv_std = lax.rsqrt(variance + EPSILON)
    centred = (conv_vals - mean_val) * inv_std
    scaled = centred * ln_gain[None, :]
    mixed_out = jax.nn.silu(scaled).astype(jnp.bfloat16)
    grad_rows = lax.dot_general(
        full_grad, mixed_out, (((0,), (0,)), ((), ())), preferred_element_type=jnp.float32
    ).astype(jnp.bfloat16)
    grad_out = (
        lax.psum_scatter(grad_rows, "sp", scatter_dimension=0, tiled=True).astype(jnp.float32).T
    )
    mixed_back = lax.dot_general(
        full_grad, w_out, (((1,), (1,)), ((), ())), preferred_element_type=jnp.float32
    )
    norm_in = mixed_back * silu_slope(scaled) * ln_gain[None, :]
    norm_total, norm_cross = group_sum(
        (jnp.sum(norm_in, axis=1), jnp.sum(norm_in * centred, axis=1)), "tp", 2
    )
    conv_back = inv_std * (
        norm_in - (norm_total / channels)[:, None] - centred * (norm_cross / channels)[:, None]
    )
    next_rim = shifted(conv_back[: tap_count - 1], "sp", -1)
    padded = jnp.concatenate([conv_back, next_rim], axis=0)
    glu_back = jnp.zeros(conv_back.shape, jnp.float32)
    for tap_index in range(tap_count):
        offset = tap_count - 1 - tap_index
        glu_back = glu_back + conv_taps[tap_index][None, :] * padded[offset : offset + tok_rows]
    gate_sigma = jax.nn.sigmoid(gate_in.astype(jnp.float32))
    value_grad = (glu_back * gate_sigma).astype(jnp.bfloat16)
    gate_grad = (glu_back * value_in.astype(jnp.float32) * gate_sigma * (1.0 - gate_sigma)).astype(
        jnp.bfloat16
    )
    return (grad_gate[None], grad_up[None], grad_down[None], grad_out, value_grad, gate_grad)


def solution(mesh):
    return jax.shard_map(
        per_device,
        mesh=mesh,
        in_specs=(
            P("sp", "tp"),
            P("sp", "tp"),
            P("tp"),
            P("sp", None),
            P("sp", None),
            P("sp", None, "tp"),
            P("sp", None, "tp"),
            P("sp", "tp", None),
            P("sp", "tp"),
            P("sp", "tp"),
            P("sp", "tp"),
            P("tp"),
            P(None, "tp"),
            P("tp", None),
        ),
        out_specs=(
            P("sp", None, "tp"),
            P("sp", None, "tp"),
            P("sp", "tp", None),
            P("tp", "sp"),
            P("sp", "tp"),
            P("sp", "tp"),
        ),
        check_vma=False,
    )
```
